32 devices in a mesh: gr: 2 (over x), fs: 4 (over z), tp: 4 (over y, core).
Axes of the slice: x: 2, y: 2, z: 4, core: 2. Of those that a mesh axis runs over, the one named last changes fastest.
Arguments:
- prompt: bfloat16 [4096, 2048], P(('gr', 'fs', 'tp')), may hold values from -6 to 6
- train_gate: float32 [16, 2048, 256], P(None, ('gr', 'fs'), 'tp'), may hold values from -0.125 to 0.125
- train_up: float32 [16, 2048, 256], P(None, ('gr', 'fs'), 'tp'), may hold values from -0.125 to 0.125
- train_down: float32 [16, 256, 2048], P(None, 'tp', ('gr', 'fs')), may hold values from -0.375 to 0.375
- train_shared_gate: float32 [2048, 256], P(('gr', 'fs'), 'tp'), may hold values from -0.125 to 0.125
- train_shared_up: float32 [2048, 256], P(('gr', 'fs'), 'tp'), may hold values from -0.125 to 0.125
- train_shared_down: float32 [256, 2048], P('tp', ('gr', 'fs')), may hold values from -0.375 to 0.375
- norm_gain: float32 [2048], P(('gr', 'fs')), may hold values from 0.1 to 1.9
- expert_ids: int32 [4096, 8], P(('gr', 'fs', 'tp')), may hold values from 0 to 15, all different within a row; in each aligned block of 128 rows (0 to 127, 128 to 255, ...) at most 65 rows name the same one
- route_weight: float32 [4096, 8], P(('gr', 'fs', 'tp')), may hold values from 0.05 to 0.6
Outputs:
- serve_gate: bfloat16 [16, 2048, 256], P(('fs', 'tp'))
- serve_up: bfloat16 [16, 2048, 256], P(('fs', 'tp'))
- serve_down: bfloat16 [16, 256, 2048], P(('fs', 'tp'))
- serve_shared_gate: bfloat16 [2048, 256], P(None, 'tp')
- serve_shared_up: bfloat16 [2048, 256], P(None, 'tp')
- serve_shared_down: bfloat16 [256, 2048], P('tp')
- mixed_out: bfloat16 [4096, 2048], P(('gr', 'fs', 'tp'))
The draws below stay inside these ranges and needn't reach their ends.
Inputs may be any that keep to these rules, and one draw needn't show every extreme that they name: `expert_ids`: each row names 8 different experts. Among the rows of one device no expert is named by more than 65 rows, and in some device's rows one expert is named by exactly 65.
All inputs are finite; a program needn't handle non-finite values.
Results may differ from the reference program's by a relative error of at most 0.012.
Values may be sent and summed in bfloat16 or wider, within the bound.
No kernel may reach another device: no remote copies, remote signals or barrier semaphores. Data moves between devices by JAX's collectives and lax.ppermute only.
A program may use at most 128 MiB of HBM per device.

```python
import math
import jax
import jax.numpy as jnp
import numpy as np
from jax import lax

D = 2048
F = 256
SHARED = 256
TOP = 8
TOK_DEV = 128
EXPERTS = 16
SHARED_BLK = 64
CAP = 65
TOKENS = 4096
N_TP = 4


def steps_of(own_key, shape, shards, least, top_value):
    level, own = 1.0, jax.random.fold_in(own_key, 6)
    for position, shards_of in shards:
        heights = jnp.exp(jax.random.uniform(jax.random.fold_in(own, position), (shards_of,), jnp.float32, least / len(shards), top_value / len(shards)))
        level = level * jnp.repeat(heights, shape[position] // shards_of).reshape([-1 if axis == position else 1 for axis in range(len(shape))])
    return level


def shared_out(rng, own, number, rows, count, top, reach, lean):
    sequence = jax.random.permutation(rng, count)
    heavy_load, ordinary = load_shares(count, rows * top, reach, lean, True), load_shares(count, rows * top, reach, lean, False)
    places = jnp.arange(count)

    def named(sizes, turn):
        used = int((sizes > 0).sum())
        fixed = max(1, used // 4)
        shifted = fixed + (places - fixed + turn * (used - fixed)) % max(1, count - fixed)
        return jnp.zeros((count,), jnp.int32).at[sequence[jnp.where(places < fixed, places, shifted)]].set(jnp.asarray(sizes, jnp.int32))

    sizes = jnp.where(number % 4 == 0, named(heavy_load, number // 4), named(ordinary, number - number // 4 - 1))
    mixed = jax.random.permutation(jax.random.fold_in(own, 3), count)
    source_of, receiver = mixed[0:count // 2 * 2:2], mixed[1:count // 2 * 2:2]
    margin = jnp.minimum(sizes[source_of] - 1, reach - sizes[receiver]) // 2
    margin = jnp.where((source_of == sequence[0]) | (receiver == sequence[0]) | (sizes[receiver] == 0), 0, jnp.maximum(margin, 0))
    shifted = jax.random.randint(jax.random.fold_in(own, 4), (count // 2,), 0, 1 << 20) % (margin + 1)
    sizes = sizes.at[source_of].add(-shifted).at[receiver].add(shifted)
    items = jnp.searchsorted(jnp.cumsum(sizes), jnp.arange(rows * top), side="right").astype(jnp.int32)
    table = items.reshape(top, rows).T
    table = table[jax.random.permutation(jax.random.fold_in(own, 1), rows)]
    turn = jax.random.randint(jax.random.fold_in(own, 2), (rows, 1), 0, top)
    return jnp.take_along_axis(table, (jnp.arange(top)[None, :] + turn) % top, axis=1)


def load_shares(count, total, reach, skew, full):
    portions = [(1 << 20) // math.isqrt(rank ** skew) + 1 for rank in range(1, count + 1)]
    largest = reach if full else min(reach, max(-(-total // count), total * portions[0] // sum(portions)))
    least = 1 if total - largest >= count - 1 else 0
    given, rest = [largest] + [least] * (count - 1), total - largest - least * (count - 1)
    while rest > 0:
        free = [i for i in range(1, count) if given[i] < largest] or [i for i in range(1, count) if given[i] < reach]
        pool, remaining = sum([portions[i] for i in free]), rest
        for i in free:
            more = min(reach - given[i], max(1, remaining * portions[i] // pool), rest)
            given[i] = given[i] + more
            rest = rest - more
    return np.array(given)


def bell_draw(key, extent, deviation, reach, shards=(), kind=jnp.bfloat16):
    loudness = steps_of(key, extent, shards, -0.22, 0.18) if shards else 1.0
    array = jax.random.normal(key, extent, jnp.float32) * deviation * loudness
    return jnp.minimum(jnp.maximum(array, -reach), reach).astype(kind)


def setup_inputs(seed: int = 0) -> dict:
    keys = jax.random.split(jax.random.key(seed), 11)
    prompt = bell_draw(keys[0], (TOKENS, D), 1.0, 6.0, ((0, 32),))
    train_gate = bell_draw(keys[1], (EXPERTS, D, F), D ** -0.5, 0.125, ((1, 8), (2, 4)), jnp.float32)
    train_up = bell_draw(keys[2], (EXPERTS, D, F), D ** -0.5, 0.125, ((1, 8), (2, 4)), jnp.float32)
    train_down = bell_draw(keys[3], (EXPERTS, F, D), F ** -0.5, 0.375, ((1, 4), (2, 8)), jnp.float32)
    train_shared_gate = bell_draw(keys[4], (D, SHARED), D ** -0.5, 0.125, ((0, 8), (1, 4)), jnp.float32)
    train_shared_up = bell_draw(keys[5], (D, SHARED), D ** -0.5, 0.125, ((0, 8), (1, 4)), jnp.float32)
    train_shared_down = bell_draw(keys[6], (SHARED, D), SHARED ** -0.5, 0.375, ((0, 4), (1, 8)), jnp.float32)
    norm_gain = jnp.clip(1.0 + 0.18 * jax.random.normal(keys[7], (D,), jnp.float32), 0.1, 1.9)
    expert_ids_keys = jax.random.split(jax.random.fold_in(keys[8], 1), TOKENS // TOK_DEV)
    expert_ids_turns = jax.random.permutation(jax.random.fold_in(keys[8], 3), TOKENS // TOK_DEV)
    expert_ids = jax.vmap(lambda own, number: shared_out(jax.random.fold_in(keys[8], 2), own, number, TOK_DEV, EXPERTS, TOP, CAP, 1))(expert_ids_keys, expert_ids_turns).reshape((TOKENS, TOP))
    route_weight = jnp.clip(0.05 + 0.55 * jax.random.uniform(keys[9], (TOKENS, TOP), jnp.float32) ** steps_of(keys[9], (TOKENS, TOP), ((0, 32),), -0.2, 0.2), 0.05, 0.6)
    return {"prompt": prompt, "train_gate": train_gate, "train_up": train_up, "train_down": train_down, "train_shared_gate": train_shared_gate, "train_shared_up": train_shared_up, "train_shared_down": train_shared_down, "norm_gain": norm_gain, "expert_ids": expert_ids, "route_weight": route_weight}


eps_norm = 1e-06

def swiglu_rows(inputs, gate_w, up_w, down_w):
    gate_val = jnp.dot(inputs, gate_w, preferred_element_type=jnp.float32)
    up_val = jnp.dot(inputs, up_w, preferred_element_type=jnp.float32)
    hidden = (jax.nn.silu(gate_val) * up_val).astype(jnp.bfloat16)
    return jnp.dot(hidden, down_w, preferred_element_type=jnp.float32).astype(jnp.bfloat16)

def reference(prompt, train_gate, train_up, train_down, train_shared_gate, train_shared_up, train_shared_down, norm_gain, expert_ids, route_weight):
    gain_col = norm_gain[:, None]
    serve_gate = (train_gate * gain_col[None]).astype(jnp.bfloat16)
    serve_up = (train_up * gain_col[None]).astype(jnp.bfloat16)
    serve_down = train_down.astype(jnp.bfloat16)
    serve_shared_gate = (train_shared_gate * gain_col).astype(jnp.bfloat16)
    serve_shared_up = (train_shared_up * gain_col).astype(jnp.bfloat16)
    serve_shared_down = train_shared_down.astype(jnp.bfloat16)
    widened = prompt.astype(jnp.float32)
    normed = (widened * lax.rsqrt(lax.optimization_barrier(jnp.mean(widened * widened, axis=-1, keepdims=True)) + eps_norm)).astype(jnp.bfloat16)
    shared_act = (jax.nn.silu(jnp.dot(normed, serve_shared_gate, preferred_element_type=jnp.float32)) * jnp.dot(normed, serve_shared_up, preferred_element_type=jnp.float32)).astype(jnp.bfloat16)
    shared_sum = jnp.zeros((TOKENS, D), jnp.float32)
    for column in range(N_TP):
        first_row = column * SHARED_BLK
        partial_out = jnp.dot(shared_act[:, first_row:first_row + SHARED_BLK], serve_shared_down[first_row:first_row + SHARED_BLK], preferred_element_type=jnp.float32).astype(jnp.bfloat16)
        partial_out = lax.optimization_barrier(partial_out)
        shared_sum = shared_sum + partial_out.astype(jnp.float32)
    blocks = TOKENS // TOK_DEV
    flat_ids = expert_ids.reshape(blocks, TOK_DEV * TOP).astype(jnp.int32)
    onehot = (flat_ids[:, :, None] == jnp.arange(EXPERTS, dtype=jnp.int32)[None, None, :]).astype(jnp.int32)
    earlier = jnp.cumsum(onehot, axis=1) - onehot
    places = lax.optimization_barrier(jnp.sum(earlier * onehot, axis=-1)).astype(jnp.int32)
    block_ids = jnp.arange(blocks, dtype=jnp.int32)[:, None]
    token_ids = block_ids * TOK_DEV + jnp.arange(TOK_DEV * TOP, dtype=jnp.int32)[None, :] // TOP
    target = ((flat_ids * blocks + block_ids) * CAP + places).reshape(-1).astype(jnp.int32)
    row_table = jnp.full((EXPERTS * blocks * CAP,), TOKENS, jnp.int32).at[target].set(token_ids.reshape(-1).astype(jnp.int32)).reshape(EXPERTS, blocks * CAP)
    row_weights = jnp.zeros((EXPERTS * blocks * CAP,), jnp.float32).at[target].set(route_weight.reshape(-1)).reshape(EXPERTS, blocks * CAP)
    padded_rows = jnp.concatenate([normed, jnp.zeros((1, D), jnp.bfloat16)], axis=0)

    def add_expert(totals, expert_data):
        rows_index, weights_here, gate_w, up_w, down_w = expert_data
        outputs = swiglu_rows(padded_rows[rows_index], gate_w, up_w, down_w)
        return (totals.at[rows_index].add(weights_here[:, None] * outputs.astype(jnp.float32)), None)
    totals, _ = lax.scan(add_expert, jnp.zeros((TOKENS + 1, D), jnp.float32), (row_table, row_weights, serve_gate, serve_up, serve_down))
    mixed_out = (totals[:TOKENS] + shared_sum).astype(jnp.bfloat16)
    return (serve_gate, serve_up, serve_down, serve_shared_gate, serve_shared_up, serve_shared_down, mixed_out)
```

```python
import jax
import jax.numpy as jnp
from jax import lax
from jax.sharding import PartitionSpec as P

eps_norm = 1e-06
row_tile = 8


def to_owners(pieces):
    count, kinds, hidden_part, width_part = pieces.shape
    fs, tp = lax.axis_size("fs"), lax.axis_size("tp")
    pieces = lax.all_to_all(pieces, ("fs", "tp"), split_axis=0, concat_axis=0, tiled=True)
    pieces = pieces.reshape(fs, tp, kinds, hidden_part, width_part)
    pieces = pieces.transpose(2, 1, 3, 0, 4).reshape(kinds, tp * hidden_part, fs * width_part)
    return lax.all_gather(pieces, "gr", axis=2, tiled=True)


def dot_last(left, right):
    return lax.dot_general(left, right, (((1,), (1,)), ((), ())), preferred_element_type=jnp.float32)


def gated(rows, gate_up):
    both = dot_last(rows, gate_up)
    hidden = both.shape[1] // 2
    return jax.nn.silu(both[:, :hidden]) * both[:, hidden:]


def dense_mix(normed, expert_ids, route_weight, gate_up, lowered, shared_gate_up, shared_down):
    fs, tp = lax.axis_size("fs"), lax.axis_size("tp")
    expert_count = fs * tp
    row_count, model_width = normed.shape
    named = expert_ids[None, :, :] == jnp.arange(expert_count, dtype=jnp.int32)[:, None, None]
    weights = jnp.sum(jnp.where(named, route_weight[None], 0.0), axis=2)
    high = lax.reduce_precision(weights, 8, 7)
    coded = jnp.stack((high, weights - high)).astype(jnp.bfloat16).reshape(-1)
    extra = -(-coded.size // (model_width * row_tile)) * row_tile
    coded = jnp.pad(coded, (0, extra * model_width - coded.size)).reshape(extra, model_width)
    block = lax.all_gather(jnp.concatenate((normed, coded), axis=0), ("fs", "tp"), axis=0)
    height = row_count + extra
    mine = lax.axis_index("fs") * tp + lax.axis_index("tp")
    sent = block[:, row_count:].reshape(expert_count, -1)[:, : 2 * expert_count * row_count]
    sent = sent.reshape(expert_count, 2, expert_count, row_count)
    own = lax.dynamic_index_in_dim(sent, mine, axis=2, keepdims=False).astype(jnp.float32)
    own = (own[:, 0] + own[:, 1])[:, :, None]
    act = gated(block.reshape(-1, model_width), gate_up).reshape(expert_count, height, -1)
    act = (act[:, :row_count] * own).astype(jnp.bfloat16)
    near = lax.dynamic_slice_in_dim(block, lax.axis_index("fs") * tp, tp, axis=0)
    shared_act = gated(near.reshape(-1, model_width), shared_gate_up).astype(jnp.bfloat16)
    shared_act = shared_act.reshape(tp, height, -1)[:, :row_count]
    placed = jnp.zeros((expert_count, row_count, shared_act.shape[2]), jnp.bfloat16)
    placed = lax.dynamic_update_slice_in_dim(placed, shared_act, lax.axis_index("fs") * tp, axis=0)
    act = jnp.concatenate((act, placed), axis=2).reshape(expert_count * row_count, -1)
    down = jnp.concatenate((lowered, shared_down), axis=0)
    partial = jnp.dot(act, down, preferred_element_type=jnp.float32).astype(jnp.bfloat16)
    return lax.psum_scatter(partial, ("fs", "tp"), scatter_dimension=0, tiled=True)


def sparse_mix(normed, expert_ids, route_weight, gate_up, lowered, shared_gate_up, shared_down):
    block_rows = lax.all_gather(normed, "tp", axis=0, tiled=True)
    shared_act = gated(block_rows, shared_gate_up).astype(jnp.bfloat16)
    shared_sum = lax.psum_scatter(
        jnp.dot(shared_act, shared_down, preferred_element_type=jnp.float32).astype(jnp.bfloat16),
        "tp",
        scatter_dimension=0,
        tiled=True,
    ).astype(jnp.float32)
    row_count, model_width = normed.shape
    top_count = expert_ids.shape[1]
    expert_count = lax.axis_size("fs") * lax.axis_size("tp")
    capacity = row_count * top_count // expert_count + 1
    flat_ids = expert_ids.reshape(-1)
    onehot = (flat_ids[:, None] == jnp.arange(expert_count, dtype=jnp.int32)[None, :]).astype(
        jnp.int32
    )
    earlier = jnp.cumsum(onehot, axis=0) - onehot
    places = jnp.sum(earlier * onehot, axis=1)
    slot_ids = (flat_ids * capacity + places).reshape(row_count, top_count)
    slot_range = jnp.arange(expert_count * capacity, dtype=jnp.int32)
    dispatch = jnp.any(slot_range[:, None, None] == slot_ids[None, :, :], axis=-1).astype(
        jnp.bfloat16
    )
    outgoing = jnp.dot(dispatch, normed, preferred_element_type=jnp.float32).astype(jnp.bfloat16)
    outgoing = outgoing.reshape(expert_count, capacity, model_width)
    arrived = lax.all_to_all(outgoing, ("fs", "tp"), split_axis=0, concat_axis=0, tiled=True)
    source_count, slot_count, width_here = arrived.shape
    arrived_rows = arrived.reshape(source_count * slot_count, width_here)
    hidden = gated(arrived_rows, gate_up).astype(jnp.bfloat16)
    result = jnp.dot(hidden, lowered, preferred_element_type=jnp.float32).astype(jnp.bfloat16)
    result = result.reshape(source_count, slot_count, width_here)
    returned = lax.all_to_all(result, ("fs", "tp"), split_axis=0, concat_axis=0, tiled=True)
    picked = returned.reshape(expert_count * capacity, model_width)[slot_ids]
    routed = jnp.sum(route_weight[:, :, None] * picked.astype(jnp.float32), axis=1)
    return (routed + shared_sum).astype(jnp.bfloat16)


def body(
    prompt,
    train_gate,
    train_up,
    train_down,
    train_shared_gate,
    train_shared_up,
    train_shared_down,
    norm_gain,
    expert_ids,
    route_weight,
):
    widened = prompt.astype(jnp.float32)
    normed = (
        widened * lax.rsqrt(jnp.mean(widened * widened, axis=-1, keepdims=True) + eps_norm)
    ).astype(jnp.bfloat16)
    gained_gate = jnp.swapaxes(train_gate, 1, 2) * norm_gain
    gained_up = jnp.swapaxes(train_up, 1, 2) * norm_gain
    stacked = to_owners(jnp.stack((gained_gate, gained_up), axis=1).astype(jnp.bfloat16))
    lowered = to_owners(train_down.astype(jnp.bfloat16)[:, None])
    shared = jnp.stack(
        (
            train_shared_gate.T * norm_gain,
            train_shared_up.T * norm_gain,
            train_shared_down,
            jnp.zeros_like(train_shared_down),
        )
    ).astype(jnp.bfloat16)
    shared = lax.all_gather(shared, ("gr", "fs"), axis=0)
    shared = shared[:, :3].transpose(1, 2, 0, 3).reshape(3, train_shared_down.shape[0], -1)
    model_width = prompt.shape[1]
    mix = dense_mix if lax.axis_size("fs") * lax.axis_size("tp") <= 2 * expert_ids.shape[1] else sparse_mix
    mixed_out = mix(
        normed,
        expert_ids,
        route_weight,
        stacked.reshape(-1, model_width),
        lowered[0],
        shared[:2].reshape(-1, model_width),
        shared[2],
    )
    return (
        jnp.swapaxes(stacked[:1], 1, 2),
        jnp.swapaxes(stacked[1:], 1, 2),
        lowered,
        shared[0].T,
        shared[1].T,
        shared[2],
        mixed_out,
    )


def solution(mesh):
    placed = (
        P(("gr", "fs", "tp"), None),
        P(None, ("gr", "fs"), "tp"),
        P(None, ("gr", "fs"), "tp"),
        P(None, "tp", ("gr", "fs")),
        P(("gr", "fs"), "tp"),
        P(("gr", "fs"), "tp"),
        P("tp", ("gr", "fs")),
        P(("gr", "fs")),
        P(("gr", "fs", "tp"), None),
        P(("gr", "fs", "tp"), None),
    )
    return jax.shard_map(
        body,
        mesh=mesh,
        in_specs=placed,
        out_specs=(
            P(("fs", "tp"), None, None),
            P(("fs", "tp"), None, None),
            P(("fs", "tp"), None, None),
            P(None, "tp"),
            P(None, "tp"),
            P("tp", None),
            P(("gr", "fs", "tp"), None),
        ),
        check_vma=False,
    )
```

```python
import jax
import jax.numpy as jnp
from jax import lax
from jax.sharding import PartitionSpec as P

eps_norm = 1e-06
row_tile = 8


def to_owners(pieces):
    count, kinds, hidden_part, width_part = pieces.shape
    fs, tp = lax.axis_size("fs"), lax.axis_size("tp")
    pieces = lax.all_to_all(pieces, ("fs", "tp"), split_axis=0, concat_axis=0, tiled=True)
    pieces = pieces.reshape(fs, tp, kinds, hidden_part, width_part)
    return pieces.transpose(2, 1, 3, 0, 4).reshape(kinds * tp * hidden_part, fs * width_part)


def join_groups(pieces):
    if lax.axis_size("gr") != 2:
        return lax.all_gather(pieces, "gr", axis=1, tiled=True)
    other = lax.ppermute(pieces, "gr", [(0, 1), (1, 0)])
    first = lax.axis_index("gr") == 0
    return jnp.concatenate(
        (jnp.where(first, pieces, other), jnp.where(first, other, pieces)), axis=1
    )


def dot_last(left, right):
    return lax.dot_general(left, right, (((1,), (1,)), ((), ())), preferred_element_type=jnp.float32)


def gated(rows, gate_up):
    both = dot_last(rows, gate_up)
    hidden = both.shape[1] // 2
    return jax.nn.silu(both[:, :hidden]) * both[:, hidden:]


def dense_mix(normed, expert_ids, route_weight, gate_up, lowered, shared_gate_up, shared_down):
    fs, tp = lax.axis_size("fs"), lax.axis_size("tp")
    expert_count = fs * tp
    row_count, model_width = normed.shape
    named = expert_ids[None, :, :] == jnp.arange(expert_count, dtype=jnp.int32)[:, None, None]
    weights = jnp.sum(jnp.where(named, route_weight[None], 0.0), axis=2)
    high = lax.reduce_precision(weights, 8, 7)
    coded = jnp.stack((high, weights - high)).astype(jnp.bfloat16).reshape(-1)
    extra = -(-coded.size // (model_width * row_tile)) * row_tile
    coded = jnp.pad(coded, (0, extra * model_width - coded.size)).reshape(extra, model_width)
    block = lax.all_gather(jnp.concatenate((normed, coded), axis=0), ("fs", "tp"), axis=0)
    height = row_count + extra
    mine = lax.axis_index("fs") * tp + lax.axis_index("tp")
    sent = block[:, row_count:].reshape(expert_count, -1)[:, : 2 * expert_count * row_count]
    sent = sent.reshape(expert_count, 2, expert_count, row_count)
    own = lax.dynamic_index_in_dim(sent, mine, axis=2, keepdims=False).astype(jnp.float32)
    own = (own[:, 0] + own[:, 1])[:, :, None]
    act = gated(block.reshape(-1, model_width), gate_up).reshape(expert_count, height, -1)
    act = (act[:, :row_count] * own).astype(jnp.bfloat16)
    near = lax.dynamic_slice_in_dim(block, lax.axis_index("fs") * tp, tp, axis=0)
    shared_act = gated(near.reshape(-1, model_width), shared_gate_up).astype(jnp.bfloat16)
    shared_act = shared_act.reshape(tp, height, -1)[:, :row_count]
    placed = jnp.zeros((expert_count, row_count, shared_act.shape[2]), jnp.bfloat16)
    placed = lax.dynamic_update_slice_in_dim(placed, shared_act, lax.axis_index("fs") * tp, axis=0)
    act = jnp.concatenate((act, placed), axis=2).reshape(expert_count * row_count, -1)
    down = jnp.concatenate((lowered, shared_down), axis=0)
    partial = jnp.dot(act, down, preferred_element_type=jnp.float32).astype(jnp.bfloat16)
    return lax.psum_scatter(partial, ("fs", "tp"), scatter_dimension=0, tiled=True)


def sparse_mix(normed, expert_ids, route_weight, gate_up, lowered, shared_gate_up, shared_down):
    block_rows = lax.all_gather(normed, "tp", axis=0, tiled=True)
    shared_act = gated(block_rows, shared_gate_up).astype(jnp.bfloat16)
    shared_sum = lax.psum_scatter(
        jnp.dot(shared_act, shared_down, preferred_element_type=jnp.float32).astype(jnp.bfloat16),
        "tp",
        scatter_dimension=0,
        tiled=True,
    ).astype(jnp.float32)
    row_count, model_width = normed.shape
    top_count = expert_ids.shape[1]
    expert_count = lax.axis_size("fs") * lax.axis_size("tp")
    capacity = row_count * top_count // expert_count + 1
    flat_ids = expert_ids.reshape(-1)
    onehot = (flat_ids[:, None] == jnp.arange(expert_count, dtype=jnp.int32)[None, :]).astype(
        jnp.int32
    )
    earlier = jnp.cumsum(onehot, axis=0) - onehot
    places = jnp.sum(earlier * onehot, axis=1)
    slot_ids = (flat_ids * capacity + places).reshape(row_count, top_count)
    slot_range = jnp.arange(expert_count * capacity, dtype=jnp.int32)
    dispatch = jnp.any(slot_range[:, None, None] == slot_ids[None, :, :], axis=-1).astype(
        jnp.bfloat16
    )
    outgoing = jnp.dot(dispatch, normed, preferred_element_type=jnp.float32).astype(jnp.bfloat16)
    outgoing = outgoing.reshape(expert_count, capacity, model_width)
    arrived = lax.all_to_all(outgoing, ("fs", "tp"), split_axis=0, concat_axis=0, tiled=True)
    source_count, slot_count, width_here = arrived.shape
    arrived_rows = arrived.reshape(source_count * slot_count, width_here)
    hidden = gated(arrived_rows, gate_up).astype(jnp.bfloat16)
    result = jnp.dot(hidden, lowered, preferred_element_type=jnp.float32).astype(jnp.bfloat16)
    result = result.reshape(source_count, slot_count, width_here)
    returned = lax.all_to_all(result, ("fs", "tp"), split_axis=0, concat_axis=0, tiled=True)
    picked = returned.reshape(expert_count * capacity, model_width)[slot_ids]
    routed = jnp.sum(route_weight[:, :, None] * picked.astype(jnp.float32), axis=1)
    return (routed + shared_sum).astype(jnp.bfloat16)


def body(
    prompt,
    train_gate,
    train_up,
    train_down,
    train_shared_gate,
    train_shared_up,
    train_shared_down,
    norm_gain,
    expert_ids,
    route_weight,
):
    widened = prompt.astype(jnp.float32)
    normed = (
        widened * lax.rsqrt(jnp.mean(widened * widened, axis=-1, keepdims=True) + eps_norm)
    ).astype(jnp.bfloat16)
    gained_gate = jnp.swapaxes(train_gate, 1, 2) * norm_gain
    gained_up = jnp.swapaxes(train_up, 1, 2) * norm_gain
    stacked = to_owners(jnp.stack((gained_gate, gained_up), axis=1).astype(jnp.bfloat16))
    stacked = join_groups(stacked).reshape(2, -1, prompt.shape[1])
    lowered = to_owners(train_down.astype(jnp.bfloat16)[:, None])
    shared = jnp.concatenate(
        (train_shared_gate.T * norm_gain, train_shared_up.T * norm_gain, train_shared_down)
    ).astype(jnp.bfloat16)
    shared = jnp.broadcast_to(shared[None], (lax.axis_size("fs"),) + shared.shape)
    shared = lax.all_to_all(shared, "fs", split_axis=0, concat_axis=0, tiled=True)
    shared = shared.transpose(1, 0, 2).reshape(shared.shape[1], -1)
    rest = join_groups(jnp.concatenate((lowered, shared), axis=0))
    lowered = rest[None, : lowered.shape[0]]
    shared = rest[lowered.shape[1] :].reshape(3, -1, prompt.shape[1])
    model_width = prompt.shape[1]
    mix = dense_mix if lax.axis_size("fs") * lax.axis_size("tp") <= 2 * expert_ids.shape[1] else sparse_mix
    mixed_out = mix(
        normed,
        expert_ids,
        route_weight,
        stacked.reshape(-1, model_width),
        lowered[0],
        shared[:2].reshape(-1, model_width),
        shared[2],
    )
    return (
        jnp.swapaxes(stacked[:1], 1, 2),
        jnp.swapaxes(stacked[1:], 1, 2),
        lowered,
        shared[0].T,
        shared[1].T,
        shared[2],
        mixed_out,
    )


def solution(mesh):
    placed = (
        P(("gr", "fs", "tp"), None),
        P(None, ("gr", "fs"), "tp"),
        P(None, ("gr", "fs"), "tp"),
        P(None, "tp", ("gr", "fs")),
        P(("gr", "fs"), "tp"),
        P(("gr", "fs"), "tp"),
        P("tp", ("gr", "fs")),
        P(("gr", "fs")),
        P(("gr", "fs", "tp"), None),
        P(("gr", "fs", "tp"), None),
    )
    return jax.shard_map(
        body,
        mesh=mesh,
        in_specs=placed,
        out_specs=(
            P(("fs", "tp"), None, None),
            P(("fs", "tp"), None, None),
            P(("fs", "tp"), None, None),
            P(None, "tp"),
            P(None, "tp"),
            P("tp", None),
            P(("gr", "fs", "tp"), None),
        ),
        check_vma=False,
    )
```
